32 devices in a mesh: kv: 4 (over y, x), tp: 8 (over z, core).
Axes of the slice: x: 2, y: 2, z: 4, core: 2. Of those that a mesh axis runs over, the one named last changes fastest.
Arguments:
- tokens: bfloat16 [64, 4096], P(None, ('kv', 'tp')), may hold values from -6 to 6
- memory: float32 [64, 16, 256, 128], P('kv', 'tp'), may hold values from -6 to 6
- normalizer: float32 [64, 16, 128], P('kv', 'tp'), may hold values from -6 to 6
- stabilizer: float32 [64, 16], P('kv', 'tp'), may hold values from -4 to 4
- first_gain: float32 [4096], replicated, may hold values from 0.1 to 1.9
- first_gate: bfloat16 [4096, 12288], P('kv', 'tp'), may hold values from -0.09375 to 0.09375
- first_up: bfloat16 [4096, 12288], P('kv', 'tp'), may hold values from -0.09375 to 0.09375
- first_down: bfloat16 [12288, 4096], P('tp', 'kv'), may hold values from -0.078125 to 0.078125
- mixer_gain: float32 [4096], replicated, may hold values from 0.1 to 1.9
- query_weight: bfloat16 [4096, 2048], P(None, 'tp'), may hold values from -0.09375 to 0.09375
- key_weight: bfloat16 [4096, 2048], P(None, 'tp'), may hold values from -0.09375 to 0.09375
- value_weight: bfloat16 [4096, 4096], P(None, 'tp'), may hold values from -0.09375 to 0.09375
- input_weight: bfloat16 [4096, 16], replicated, may hold values from -0.09375 to 0.09375
- forget_weight: bfloat16 [4096, 16], replicated, may hold values from -0.09375 to 0.09375
- forget_bias: float32 [16], P('tp'), may hold values from -2 to 4
- output_weight: bfloat16 [4096, 4096], P('tp'), may hold values from -0.09375 to 0.09375
- last_gain: float32 [4096], replicated, may hold values from 0.1 to 1.9
- last_gate: bfloat16 [4096, 12288], P('kv', 'tp'), may hold values from -0.09375 to 0.09375
- last_up: bfloat16 [4096, 12288], P('kv', 'tp'), may hold values from -0.09375 to 0.09375
- last_down: bfloat16 [12288, 4096], P('tp', 'kv'), may hold values from -0.078125 to 0.078125
Outputs:
- result: bfloat16 [64, 4096], P(None, ('kv', 'tp'))
- new_memory: float32 [64, 16, 256, 128], P('kv', 'tp')
- new_normalizer: float32 [64, 16, 128], P('kv', 'tp')
- new_stabilizer: float32 [64, 16], P('kv', 'tp')
The draws below stay inside these ranges and needn't reach their ends.
All inputs are finite; a program needn't handle non-finite values.
Results may differ from the reference program's by a relative error of at most 0.025.
Values may be sent and summed in bfloat16 or wider, within the bound.
A program may use at most 128 MiB of HBM per device.

```python
import jax
import jax.numpy as jnp
from jax import lax

D = 4096
FF = 12288
HEADS = 16
DK = 128
DV = 256
BATCH = 64


def strengthened(entries, own_key, source, target, blocks, factor):
    def block_of(dim):
        return (jnp.arange(entries.shape[dim]) // (entries.shape[dim] // blocks)).reshape((-1,) + (1,) * (entries.ndim - 1 - dim))

    first = jax.random.permutation(own_key, blocks)[block_of(target)]
    other_side = (block_of(target) + blocks // 2) % blocks
    return jnp.where((block_of(source) == first) | (block_of(source) == other_side), factor * entries, entries)


def block_scale(key, extent, cuts, smallest, top_value):
    def one(axis_at, blocks):
        heights = jax.random.uniform(jax.random.fold_in(jax.random.fold_in(key, 6), axis_at), (blocks,), jnp.float32, smallest / len(cuts), top_value / len(cuts))
        return jnp.repeat(jnp.exp(heights), extent[axis_at] // blocks).reshape((-1,) + (1,) * (len(extent) - axis_at - 1))

    loudness = one(*cuts[0])
    for cut in cuts[1:]:
        loudness = loudness * one(*cut)
    return loudness


def normal_values(own_key, shape, deviation, most, pieces=(), held_as=jnp.bfloat16):
    level = block_scale(own_key, shape, pieces, -0.22, 0.18) if pieces else 1.0
    drawn = jax.random.normal(own_key, shape, jnp.float32) * deviation * level
    return jnp.minimum(jnp.maximum(drawn, -most), most).astype(held_as)


def gaussian_with(stream_key, dims, spread, reach, cuts, heavy, dtype=jnp.bfloat16):
    values = spread * jax.random.normal(stream_key, dims, jnp.float32)
    if cuts:
        values = values * block_scale(stream_key, dims, cuts, -0.22, 0.18)
    return jnp.clip(strengthened(values, jax.random.fold_in(stream_key, 3), *heavy), -reach, reach).astype(dtype)


def setup_inputs(seed: int = 0) -> dict:
    arg_keys = jax.random.split(jax.random.key(seed), 21)
    tokens = normal_values(arg_keys[0], (BATCH, D), 1.0, 6.0, ((1, 32),))
    memory = normal_values(arg_keys[1], (BATCH, HEADS, DV, DK), 1.0, 6.0, ((0, 4), (1, 8)), jnp.float32)
    normalizer = normal_values(arg_keys[2], (BATCH, HEADS, DK), 1.0, 6.0, ((0, 4), (1, 8)), jnp.float32)
    stabilizer = normal_values(arg_keys[3], (BATCH, HEADS), 1.0, 4.0, ((0, 4), (1, 8)), jnp.float32)
    first_gain = jnp.clip(1.0 + 0.18 * jax.random.normal(arg_keys[4], (D,), jnp.float32), 0.1, 1.9)
    first_gate = normal_values(arg_keys[5], (D, FF), D ** -0.5, 0.09375, ((0, 4), (1, 8)))
    first_up = normal_values(arg_keys[6], (D, FF), D ** -0.5, 0.09375, ((0, 4), (1, 8)))
    first_down = gaussian_with(arg_keys[7], (FF, D), FF ** -0.5, 0.078125, ((0, 8), (1, 4)), (0, 1, 8, 2.0))
    mixer_gain = jnp.clip(1.0 + 0.18 * jax.random.normal(arg_keys[8], (D,), jnp.float32), 0.1, 1.9)
    query_weight = normal_values(arg_keys[9], (D, HEADS * DK), D ** -0.5, 0.09375, ((1, 8),))
    key_weight = normal_values(arg_keys[10], (D, HEADS * DK), D ** -0.5, 0.09375, ((1, 8),))
    value_weight = normal_values(arg_keys[11], (D, HEADS * DV), D ** -0.5, 0.09375, ((1, 8),))
    input_weight = normal_values(arg_keys[12], (D, HEADS), D ** -0.5, 0.09375)
    forget_weight = normal_values(arg_keys[13], (D, HEADS), D ** -0.5, 0.09375)
    forget_bias = jnp.clip(-2.0 + 6.0 * jax.random.uniform(arg_keys[14], (HEADS,), jnp.float32) ** block_scale(arg_keys[14], (HEADS,), ((0, 8),), -0.2, 0.2), -2.0, 4.0)
    output_weight = normal_values(arg_keys[15], (HEADS * DV, D), (HEADS * DV) ** -0.5, 0.09375, ((0, 8),))
    last_gain = jnp.clip(1.0 + 0.18 * jax.random.normal(arg_keys[16], (D,), jnp.float32), 0.1, 1.9)
    last_gate = normal_values(arg_keys[17], (D, FF), D ** -0.5, 0.09375, ((0, 4), (1, 8)))
    last_up = normal_values(arg_keys[18], (D, FF), D ** -0.5, 0.09375, ((0, 4), (1, 8)))
    last_down = gaussian_with(arg_keys[19], (FF, D), FF ** -0.5, 0.078125, ((0, 8), (1, 4)), (0, 1, 8, 2.0))
    return {"tokens": tokens, "memory": memory, "normalizer": normalizer, "stabilizer": stabilizer, "first_gain": first_gain, "first_gate": first_gate, "first_up": first_up, "first_down": first_down, "mixer_gain": mixer_gain, "query_weight": query_weight, "key_weight": key_weight, "value_weight": value_weight, "input_weight": input_weight, "forget_weight": forget_weight, "forget_bias": forget_bias, "output_weight": output_weight, "last_gain": last_gain, "last_gate": last_gate, "last_up": last_up, "last_down": last_down}


EPS = 1e-06

def norm_scale(stream):
    values = stream.astype(jnp.float32)
    return lax.rsqrt(lax.optimization_barrier(jnp.mean(values * values, axis=-1, keepdims=True)) + EPS)

def gated_mlp(stream, gain, w_gate, w_up, w_down):
    scale = norm_scale(stream)
    scaled = (stream.astype(jnp.float32) * gain).astype(jnp.bfloat16)
    gate = scale * jnp.dot(scaled, w_gate, preferred_element_type=jnp.float32)
    up = scale * jnp.dot(scaled, w_up, preferred_element_type=jnp.float32)
    hidden = (jax.nn.silu(gate) * up).astype(jnp.bfloat16)
    return jnp.dot(hidden, w_down, preferred_element_type=jnp.float32)

def reference(tokens, memory, normalizer, stabilizer, first_gain, first_gate, first_up, first_down, mixer_gain, query_weight, key_weight, value_weight, input_weight, forget_weight, forget_bias, output_weight, last_gain, last_gate, last_up, last_down):
    f32 = jnp.float32
    first_sum = gated_mlp(tokens, first_gain, first_gate, first_up, first_down)
    stream_one = (tokens.astype(f32) + 0.5 * first_sum).astype(jnp.bfloat16)
    batch = tokens.shape[0]
    scale = norm_scale(stream_one)
    cell_in = (stream_one.astype(f32) * mixer_gain).astype(jnp.bfloat16)
    query = (scale * jnp.dot(cell_in, query_weight, preferred_element_type=f32) * DK ** (-0.5)).reshape(batch, HEADS, DK)
    key = (scale * jnp.dot(cell_in, key_weight, preferred_element_type=f32)).reshape(batch, HEADS, DK)
    value = (scale * jnp.dot(cell_in, value_weight, preferred_element_type=f32)).reshape(batch, HEADS, DV)
    input_pre = scale * jnp.dot(cell_in, input_weight, preferred_element_type=f32)
    log_forget = jax.nn.log_sigmoid(scale * jnp.dot(cell_in, forget_weight, preferred_element_type=f32) + forget_bias)
    carried = log_forget + stabilizer
    new_stabilizer = jnp.maximum(carried, input_pre)
    keep = jnp.exp(carried - new_stabilizer)
    admit = jnp.exp(input_pre - new_stabilizer)
    recalled = jnp.einsum('bhvd,bhd->bhv', memory, query, precision=lax.Precision.HIGHEST)
    match = lax.optimization_barrier(jnp.sum(query * key, axis=-1))
    numer = keep[..., None] * recalled + (admit * match)[..., None] * value
    denom = keep * lax.optimization_barrier(jnp.sum(normalizer * query, axis=-1)) + admit * match
    cell_out = (numer / jnp.maximum(jnp.abs(denom), 1.0)[..., None]).reshape(batch, HEADS * DV).astype(jnp.bfloat16)
    new_memory = keep[..., None, None] * memory + admit[..., None, None] * value[..., :, None] * key[..., None, :]
    new_normalizer = keep[..., None] * normalizer + admit[..., None] * key
    mixed = jnp.dot(cell_out, output_weight, preferred_element_type=f32)
    stream_two = (stream_one.astype(f32) + mixed).astype(jnp.bfloat16)
    last_sum = gated_mlp(stream_two, last_gain, last_gate, last_up, last_down)
    result = (stream_two.astype(f32) + 0.5 * last_sum).astype(jnp.bfloat16)
    return (result, new_memory, new_normalizer, new_stabilizer)
```

```python
import jax
import jax.numpy as jnp
from jax import lax
from jax.experimental import pallas as pl
from jax.experimental.pallas import tpu as pltpu
from jax.sharding import PartitionSpec as P

EPS = 1e-06
MESH = pl.DeviceIdType.MESH


def hidden_units(gate_acc, up_acc, squares, model_width):
    scale = lax.rsqrt(squares / model_width + EPS)[:, None]
    return (jax.nn.silu(scale * gate_acc) * (scale * up_acc)).astype(jnp.bfloat16)


def gated_block(block, gain, w_gate, w_up, w_down, model_width):
    f32 = jnp.float32
    width = block.shape[1]
    gain_block = lax.dynamic_slice_in_dim(gain, lax.axis_index("kv") * width, width, 0)
    values = block.astype(f32)
    scaled = (values * gain_block).astype(jnp.bfloat16)
    gate_part = jnp.dot(scaled, w_gate, preferred_element_type=f32)
    up_part = jnp.dot(scaled, w_up, preferred_element_type=f32)
    squares = jnp.sum(values * values, axis=1)
    gate_acc, up_acc, sq_total = (
        lax.psum(gate_part.astype(jnp.bfloat16), "kv").astype(jnp.float32),
        lax.psum(up_part.astype(jnp.bfloat16), "kv").astype(jnp.float32),
        lax.psum(squares.astype(jnp.bfloat16), "kv").astype(jnp.float32),
    )
    hidden = hidden_units(gate_acc, up_acc, sq_total, model_width)
    share = lax.psum_scatter(
        lax.dot_general(
            w_down, hidden, (((0,), (1,)), ((), ())), preferred_element_type=f32
        ).astype(jnp.bfloat16),
        "tp",
        scatter_dimension=0,
        tiled=True,
    ).astype(jnp.float32)
    return share.T


def body(
    tokens,
    memory,
    normalizer,
    stabilizer,
    first_gain,
    first_gate,
    first_up,
    first_down,
    mixer_gain,
    query_weight,
    key_weight,
    value_weight,
    input_weight,
    forget_weight,
    forget_bias,
    output_weight,
    last_gain,
    last_gate,
    last_up,
    last_down,
):
    f32 = jnp.float32
    model_width = first_gain.shape[0]
    rows, col_width = tokens.shape
    block = lax.all_gather(tokens, "tp", axis=1, tiled=True)
    first_share = gated_block(block, first_gain, first_gate, first_up, first_down, model_width)
    stream_one = (tokens.astype(f32) + 0.5 * first_share).astype(jnp.bfloat16)
    seq_count, head_count, value_size, key_size = memory.shape
    moved = lax.all_to_all(
        stream_one.reshape(rows, 1, col_width), "kv", split_axis=0, concat_axis=1, tiled=True
    )
    own_rows = lax.all_gather(moved, "tp", axis=2, tiled=True).reshape(seq_count, model_width)
    row_values = own_rows.astype(f32)
    scale = lax.rsqrt(jnp.mean(row_values * row_values, axis=1, keepdims=True) + EPS)
    cell_in = (row_values * mixer_gain).astype(jnp.bfloat16)
    query = (
        scale * jnp.dot(cell_in, query_weight, preferred_element_type=f32) * key_size ** (-0.5)
    ).reshape(seq_count, head_count, key_size)
    key = (scale * jnp.dot(cell_in, key_weight, preferred_element_type=f32)).reshape(
        seq_count, head_count, key_size
    )
    value = (scale * jnp.dot(cell_in, value_weight, preferred_element_type=f32)).reshape(
        seq_count, head_count, value_size
    )
    first_head = lax.axis_index("tp") * head_count
    input_all = scale * jnp.dot(cell_in, input_weight, preferred_element_type=f32)
    forget_all = scale * jnp.dot(cell_in, forget_weight, preferred_element_type=f32)
    input_pre = lax.dynamic_slice_in_dim(input_all, first_head, head_count, 1)
    log_forget = jax.nn.log_sigmoid(
        lax.dynamic_slice_in_dim(forget_all, first_head, head_count, 1) + forget_bias
    )
    carried = log_forget + stabilizer
    new_stabilizer = jnp.maximum(carried, input_pre)
    keep = jnp.exp(carried - new_stabilizer)
    admit = jnp.exp(input_pre - new_stabilizer)
    recalled = jnp.einsum("bhvd,bhd->bhv", memory, query, precision=lax.Precision.HIGHEST)
    match = jnp.sum(query * key, axis=-1)
    numer = keep[..., None] * recalled + (admit * match)[..., None] * value
    denom = keep * jnp.sum(normalizer * query, axis=-1) + admit * match
    cell_out = (
        (numer / jnp.maximum(jnp.abs(denom), 1.0)[..., None])
        .reshape(seq_count, head_count * value_size)
        .astype(jnp.bfloat16)
    )
    new_memory = (
        keep[..., None, None] * memory
        + admit[..., None, None] * value[..., :, None] * key[..., None, :]
    )
    new_normalizer = keep[..., None] * normalizer + admit[..., None] * key
    partial_heads = jnp.dot(cell_out, output_weight, preferred_element_type=f32)
    mixed = lax.psum(partial_heads.astype(jnp.bfloat16), "tp").astype(jnp.float32)
    rows_two = (row_values + mixed).astype(jnp.bfloat16)
    whole_two = lax.all_to_all(rows_two, "kv", split_axis=1, concat_axis=0, tiled=True)
    last_share = gated_block(whole_two, last_gain, last_gate, last_up, last_down, model_width)
    own_columns = lax.dynamic_slice_in_dim(
        whole_two, lax.axis_index("tp") * col_width, col_width, 1
    )
    result = (own_columns.astype(f32) + 0.5 * last_share).astype(jnp.bfloat16)
    return (result, new_memory, new_normalizer, new_stabilizer)


def tiles_fit(tokens, memory, first_down, kv_size, tp_size):
    rows, col_width = tokens.shape
    seqs, heads, value_size, key_size = memory.shape
    hidden = first_down.shape[0]
    return (
        col_width % 128 == 0
        and hidden % (128 * kv_size) == 0
        and seqs % 16 == 0
        and seqs * kv_size == rows
        and key_size % 128 == 0
        and value_size % 128 == 0
        and tp_size > 1
        and kv_size > 1
    )


def make_kernel(K, T, R, C, F, S, H, DK, DV):
    f32, bf16 = jnp.float32, jnp.bfloat16
    W, FQ = C * T, F // K
    D = W * K
    mlp_remote = 2 * (T - 1) + 3 * (K - 1)
    remote_count = 2 * mlp_remote + 2 * (T - 1) + 2 * (K - 1)

    def kernel(
        tokens, normalizer, stabilizer, first_gain, mixer_gain, forget_bias, last_gain,
        memory, fg, fu, fd, wq, wk, wv, wi, wf, wo, lg, lu, ld,
        result, query_out, key_out, value_out, keep_out, admit_out, stab_out,
        send_sem, recv_sem, load_sem,
        v_fg, v_fu, v_fd, v_lg, v_lu, v_ld, v_qkv, v_wi, v_wf, v_wo, v_mem,
        *bufs,
    ):
        mlp_bufs = (bufs[0:9], bufs[9:18])
        s_one, moved, rows_all, rows_val, cell_in, qkv, cell_out, part, part_in, two, two_in, s_two = bufs[18:]
        k = lax.axis_index("kv")
        t = lax.axis_index("tp")
        counter = [0]

        loads = {}

        def load(name, src, dst):
            i = len(loads)
            copy = pltpu.make_async_copy(src, dst, load_sem.at[i])
            copy.start()
            loads[name] = copy

        load("fg", fg, v_fg)
        load("fu", fu, v_fu)
        load("fd", fd, v_fd)
        load("wq", wq, v_qkv.at[:, pl.ds(0, H * DK)])
        load("wk", wk, v_qkv.at[:, pl.ds(H * DK, H * DK)])
        load("wv", wv, v_qkv.at[:, pl.ds(2 * H * DK, H * DV)])
        load("wi", wi, v_wi)
        load("wf", wf, v_wf)
        load("mem", memory, v_mem)
        load("wo", wo, v_wo)
        load("lg", lg, v_lg)
        load("lu", lu, v_lu)
        load("ld", ld, v_ld)

        barrier = pltpu.get_barrier_semaphore()
        for o in range(1, T):
            pl.semaphore_signal(barrier, inc=1, device_id=(k, lax.rem(t + o, T)), device_id_type=MESH)
        for o in range(1, K):
            pl.semaphore_signal(barrier, inc=1, device_id=(lax.rem(k + o, K), t), device_id_type=MESH)
        pl.semaphore_wait(barrier, T + K - 2)

        def send(src, dst, device):
            i = counter[0]
            counter[0] += 1
            copy = pltpu.make_async_remote_copy(
                src_ref=src, dst_ref=dst, send_sem=send_sem.at[i], recv_sem=recv_sem.at[i],
                device_id=device, device_id_type=MESH,
            )
            copy.start()
            return copy

        started = []

        def tp_to(o):
            return (k, lax.rem(t + o, T))

        def kv_to(o):
            return (lax.rem(k + o, K), t)

        def tp_from(o):
            return lax.rem(t + (T - o), T)

        def kv_from(o):
            return lax.rem(k + (K - o), K)

        def cols(at, width):
            return pl.ds(pl.multiple_of(at * width, width), width)

        def mlp(own, gain, vg, vu, vd, names, b):
            gath, scaled, sq_out, sq_in, gu_out, gu_in, hid, hid_in, down = b[:9]
            copies = [send(own, gath.at[o], tp_to(o)) for o in range(1, T)]
            squares = jnp.zeros((R, C), f32)

            def take(x, src, squares):
                values = x.astype(f32)
                at = pl.ds(pl.multiple_of((k * T + src) * C, C), C)
                scaled[:, cols(src, C)] = (values * gain[:, at]).astype(bf16)
                return squares + values * values

            squares = take(own[...], t, squares)
            for o in range(1, T):
                copies[o - 1].wait_recv()
                squares = take(gath[o], tp_from(o), squares)
            started.extend(copies)
            total = jnp.sum(squares, axis=1, keepdims=True)
            sq_out[...] = jnp.broadcast_to(total, (R, 128))
            sq_copies = [send(sq_out, sq_in.at[o], kv_to(o)) for o in range(1, K)]
            loads[names[0]].wait()
            loads[names[1]].wait()
            x = scaled[...]
            gu_copies = []
            for o in range(1, K):
                at = cols(lax.rem(k + o, K), FQ)
                gu_out[o, 0] = jnp.dot(x, vg[:, at], preferred_element_type=f32).astype(bf16)
                gu_out[o, 1] = jnp.dot(x, vu[:, at], preferred_element_type=f32).astype(bf16)
                gu_copies.append(send(gu_out.at[o], gu_in.at[o], kv_to(o)))
            at = cols(k, FQ)
            gate = jnp.dot(x, vg[:, at], preferred_element_type=f32)
            up = jnp.dot(x, vu[:, at], preferred_element_type=f32)
            for c in sq_copies:
                c.wait_recv()
            for o in range(1, K):
                total = total + sq_in[o][:, :1]
            scale = lax.rsqrt(total / D + EPS)
            for o in range(1, K):
                gu_copies[o - 1].wait_recv()
                gate = gate + gu_in[o, 0].astype(f32)
                up = up + gu_in[o, 1].astype(f32)
            gate = gate * scale
            up = up * scale
            mine = (gate / (1.0 + jnp.exp(-gate)) * up).astype(bf16)
            hid_in[0] = mine
            hid_copies = [send(hid_in.at[0], hid_in.at[o], kv_to(o)) for o in range(1, K)]
            hid[:, cols(k, FQ)] = mine
            loads[names[2]].wait()
            for o in range(1, K):
                hid_copies[o - 1].wait_recv()
                hid[:, cols(kv_from(o), FQ)] = hid_in[o]
            for c in range(0, T):
                down[c] = jnp.dot(
                    hid[...], vd[:, c * C:(c + 1) * C], preferred_element_type=f32
                ).astype(bf16)
            out_copies = [send(down.at[lax.rem(t + o, T)], gath.at[T + o], tp_to(o)) for o in range(1, T)]
            acc = down[t].astype(f32)
            for o in range(1, T):
                out_copies[o - 1].wait_recv()
                acc = acc + gath[T + o].astype(f32)
            started.extend(sq_copies + gu_copies + hid_copies + out_copies)
            return (own[...].astype(f32) + 0.5 * acc).astype(bf16)

        s_one[...] = mlp(tokens, first_gain, v_fg, v_fu, v_fd, ("fg", "fu", "fd"), mlp_bufs[0])

        move = [
            send(s_one.at[pl.ds(pl.multiple_of(lax.rem(k + o, K) * S, S), S), :], moved.at[o], kv_to(o))
            for o in range(1, K)
        ]
        moved[0] = s_one[pl.ds(pl.multiple_of(k * S, S), S), :]
        for c in move:
            c.wait_recv()
        gather = [send(moved, rows_all.at[o], tp_to(o)) for o in range(1, T)]
        squares = jnp.zeros((S, C), f32)
        for o in range(0, T):
            if o:
                gather[o - 1].wait_recv()
            for j in range(K):
                values = (rows_all[o, j] if o else moved[j]).astype(f32)
                at = cols(kv_from(j) * T + tp_from(o), C)
                rows_val[:, at] = values
                cell_in[:, at] = (values * mixer_gain[:, at]).astype(bf16)
                squares = squares + values * values
        started.extend(move + gather)
        scale = lax.rsqrt(jnp.sum(squares, axis=1, keepdims=True) / D + EPS)
        for name in ("wq", "wk", "wv", "wi", "wf"):
            loads[name].wait()
        width = 2 * H * DK + H * DV

        def project(n, carry):
            at = cols(n, 128 * 2 if width % 256 == 0 else 128)
            qkv[:, at] = scale * jnp.dot(cell_in[...], v_qkv[:, at], preferred_element_type=f32)
            return carry

        lax.fori_loop(0, width // (256 if width % 256 == 0 else 128), project, 0)
        input_all = scale * jnp.dot(cell_in[...], v_wi[...], preferred_element_type=f32)
        forget_all = scale * jnp.dot(cell_in[...], v_wf[...], preferred_element_type=f32)
        lane = lax.broadcasted_iota(jnp.int32, input_all.shape, 1)
        loads["mem"].wait()
        rowid = lax.broadcasted_iota(jnp.int32, (S, DV), 0)
        query = qkv[:, : H * DK] * DK ** (-0.5)
        key = qkv[:, H * DK : 2 * H * DK]
        value = qkv[:, 2 * H * DK :]
        query_out[...] = query
        key_out[...] = key
        value_out[...] = value
        hi = query.astype(bf16)
        lo = (query - hi.astype(f32)).astype(bf16)
        dims = (((1,), (1,)), ((), ()))
        step = 4 if S % 4 == 0 else 1

        def recall(i, acc):
            acc = list(acc)
            for h in range(H):
                qh = hi[:, h * DK : (h + 1) * DK]
                ql = lo[:, h * DK : (h + 1) * DK]
                for j in range(step):
                    m = v_mem[i * step + j, h]
                    mh = m.astype(bf16)
                    ml = (m - mh.astype(f32)).astype(bf16)
                    r = (
                        lax.dot_general(qh, mh, dims, preferred_element_type=f32)
                        + lax.dot_general(ql, mh, dims, preferred_element_type=f32)
                        + lax.dot_general(qh, ml, dims, preferred_element_type=f32)
                    )
                    acc[h] = jnp.where(rowid == i * step + j, r, acc[h])
            return tuple(acc)

        recalled = lax.fori_loop(0, S // step, recall, tuple(jnp.zeros((S, DV), f32) for _ in range(H)))
        for h in range(H):
            own_head = lane == t * H + h
            input_pre = jnp.sum(jnp.where(own_head, input_all, 0.0), axis=1, keepdims=True)
            pre = jnp.sum(jnp.where(own_head, forget_all, 0.0), axis=1, keepdims=True) + forget_bias[:, h : h + 1]
            log_forget = jnp.minimum(pre, 0.0) - jnp.log1p(jnp.exp(-jnp.abs(pre)))
            carried = log_forget + stabilizer[:, h : h + 1]
            new_stab = jnp.maximum(carried, input_pre)
            keep = jnp.exp(carried - new_stab)
            admit = jnp.exp(input_pre - new_stab)
            stab_out[:, h : h + 1] = new_stab
            keep_out[:, h : h + 1] = keep
            admit_out[:, h : h + 1] = admit
            qh = query[:, h * DK : (h + 1) * DK]
            match = jnp.sum(qh * key[:, h * DK : (h + 1) * DK], axis=1, keepdims=True)
            held = jnp.sum(qh * normalizer[:, h, :], axis=1, keepdims=True)
            numer = keep * recalled[h] + (admit * match) * value[:, h * DV : (h + 1) * DV]
            denom = keep * held + admit * match
            cell_out[:, h * DV : (h + 1) * DV] = (numer / jnp.maximum(jnp.abs(denom), 1.0)).astype(bf16)

        loads["wo"].wait()

        def spread(j, carry):
            for c in range(0, T):
                at = pl.ds(pl.multiple_of(j * W + c * C, C), C)
                part[c, j] = jnp.dot(cell_out[...], v_wo[:, at], preferred_element_type=f32).astype(bf16)
            return carry

        lax.fori_loop(0, K, spread, 0)
        mix = [send(part.at[lax.rem(t + o, T)], part_in.at[o], tp_to(o)) for o in range(1, T)]
        mixed = part[t].astype(f32)
        for o in range(1, T):
            mix[o - 1].wait_recv()
            mixed = mixed + part_in[o].astype(f32)
        for j in range(K):
            at = cols(j * T + t, C)
            two[j] = (rows_val[:, at] + mixed[j]).astype(bf16)
        back = [send(two.at[lax.rem(k + o, K)], two_in.at[o], kv_to(o)) for o in range(1, K)]
        s_two[pl.ds(pl.multiple_of(k * S, S), S), :] = two[k]
        for o in range(1, K):
            back[o - 1].wait_recv()
            s_two[pl.ds(pl.multiple_of(kv_from(o) * S, S), S), :] = two_in[o]
        started.extend(mix + back)

        result[...] = mlp(s_two, last_gain, v_lg, v_lu, v_ld, ("lg", "lu", "ld"), mlp_bufs[1])
        for c in started:
            c.wait_send()

    mlp_scratch = [
        pltpu.VMEM((2 * T, R, C), bf16),
        pltpu.VMEM((R, W), bf16),
        pltpu.VMEM((R, 128), f32),
        pltpu.VMEM((K, R, 128), f32),
        pltpu.VMEM((K, 2, R, FQ), bf16),
        pltpu.VMEM((K, 2, R, FQ), bf16),
        pltpu.VMEM((R, F), bf16),
        pltpu.VMEM((K, R, FQ), bf16),
        pltpu.VMEM((T, R, C), bf16),
    ]

    def scratch(heads_all):
        return [
            pltpu.SemaphoreType.DMA((remote_count,)),
            pltpu.SemaphoreType.DMA((remote_count,)),
            pltpu.SemaphoreType.DMA((13,)),
            pltpu.VMEM((W, F), bf16),
            pltpu.VMEM((W, F), bf16),
            pltpu.VMEM((F, W), bf16),
            pltpu.VMEM((W, F), bf16),
            pltpu.VMEM((W, F), bf16),
            pltpu.VMEM((F, W), bf16),
            pltpu.VMEM((D, 2 * H * DK + H * DV), bf16),
            pltpu.VMEM((D, heads_all), bf16),
            pltpu.VMEM((D, heads_all), bf16),
            pltpu.VMEM((H * DV, D), bf16),
            pltpu.VMEM((S, H, DV, DK), f32),
            *mlp_scratch,
            *mlp_scratch,
            pltpu.VMEM((R, C), bf16),
            pltpu.VMEM((K, S, C), bf16),
            pltpu.VMEM((T, K, S, C), bf16),
            pltpu.VMEM((S, D), f32),
            pltpu.VMEM((S, D), bf16),
            pltpu.VMEM((S, 2 * H * DK + H * DV), f32),
            pltpu.VMEM((S, H * DV), bf16),
            pltpu.VMEM((T, K, S, C), bf16),
            pltpu.VMEM((T, K, S, C), bf16),
            pltpu.VMEM((K, S, C), bf16),
            pltpu.VMEM((K, S, C), bf16),
            pltpu.VMEM((R, C), bf16),
        ]

    return kernel, scratch


def fused_body(
    tokens, memory, normalizer, stabilizer, first_gain, first_gate, first_up, first_down,
    mixer_gain, query_weight, key_weight, value_weight, input_weight, forget_weight,
    forget_bias, output_weight, last_gain, last_gate, last_up, last_down,
):
    f32 = jnp.float32
    kv_size, tp_size = lax.axis_size("kv"), lax.axis_size("tp")
    R, C = tokens.shape
    S, H, DV, DK = memory.shape
    F = first_down.shape[0]
    kernel, scratch = make_kernel(kv_size, tp_size, R, C, F, S, H, DK, DV)
    vmem, anyspace = pl.BlockSpec(memory_space=pltpu.VMEM), pl.BlockSpec(memory_space=pl.ANY)
    shape = jax.ShapeDtypeStruct
    result, query, key, value, keep, admit, new_stabilizer = pl.pallas_call(
        kernel,
        out_shape=(
            shape((R, C), jnp.bfloat16),
            shape((S, H * DK), f32),
            shape((S, H * DK), f32),
            shape((S, H * DV), f32),
            shape((S, H), f32),
            shape((S, H), f32),
            shape((S, H), f32),
        ),
        in_specs=[vmem] * 7 + [anyspace] * 13,
        out_specs=(vmem,) * 7,
        scratch_shapes=scratch(input_weight.shape[1]),
        compiler_params=pltpu.CompilerParams(
            collective_id=0, has_side_effects=True, vmem_limit_bytes=60 * 2**20
        ),
    )(
        tokens, normalizer, stabilizer, first_gain[None], mixer_gain[None], forget_bias[None], last_gain[None],
        memory, first_gate, first_up, first_down, query_weight, key_weight, value_weight,
        input_weight, forget_weight, output_weight, last_gate, last_up, last_down,
    )
    key = key.reshape(S, H, DK)
    value = value.reshape(S, H, DV)
    new_memory = (
        keep[..., None, None] * memory
        + admit[..., None, None] * value[..., :, None] * key[..., None, :]
    )
    new_normalizer = keep[..., None] * normalizer + admit[..., None] * key
    return result, new_memory, new_normalizer, new_stabilizer


def solution(mesh):
    in_specs = (
        P(None, ("kv", "tp")),
        P("kv", "tp", None, None),
        P("kv", "tp", None),
        P("kv", "tp"),
        P(),
        P("kv", "tp"),
        P("kv", "tp"),
        P("tp", "kv"),
        P(),
        P(None, "tp"),
        P(None, "tp"),
        P(None, "tp"),
        P(),
        P(),
        P("tp"),
        P("tp", None),
        P(),
        P("kv", "tp"),
        P("kv", "tp"),
        P("tp", "kv"),
    )
    out_specs = (
        P(None, ("kv", "tp")),
        P("kv", "tp", None, None),
        P("kv", "tp", None),
        P("kv", "tp"),
    )
    kv_size, tp_size = mesh.shape["kv"], mesh.shape["tp"]

    def chosen(tokens, memory, *rest):
        fits = tiles_fit(tokens, memory, rest[5], kv_size, tp_size)
        return (fused_body if fits else body)(tokens, memory, *rest)

    return jax.shard_map(chosen, mesh=mesh, in_specs=in_specs, out_specs=out_specs, check_vma=False)
```

```python
import jax
import jax.numpy as jnp
from jax import lax
from jax.experimental import pallas as pl
from jax.experimental.pallas import tpu as pltpu
from jax.sharding import PartitionSpec as P

EPS = 1e-06
MESH = pl.DeviceIdType.MESH


def hidden_units(gate_acc, up_acc, squares, model_width):
    scale = lax.rsqrt(squares / model_width + EPS)[:, None]
    return (jax.nn.silu(scale * gate_acc) * (scale * up_acc)).astype(jnp.bfloat16)


def gated_block(block, gain, w_gate, w_up, w_down, model_width):
    f32 = jnp.float32
    width = block.shape[1]
    gain_block = lax.dynamic_slice_in_dim(gain, lax.axis_index("kv") * width, width, 0)
    values = block.astype(f32)
    scaled = (values * gain_block).astype(jnp.bfloat16)
    gate_part = jnp.dot(scaled, w_gate, preferred_element_type=f32)
    up_part = jnp.dot(scaled, w_up, preferred_element_type=f32)
    squares = jnp.sum(values * values, axis=1)
    gate_acc, up_acc, sq_total = (
        lax.psum(gate_part.astype(jnp.bfloat16), "kv").astype(jnp.float32),
        lax.psum(up_part.astype(jnp.bfloat16), "kv").astype(jnp.float32),
        lax.psum(squares.astype(jnp.bfloat16), "kv").astype(jnp.float32),
    )
    hidden = hidden_units(gate_acc, up_acc, sq_total, model_width)
    share = lax.psum_scatter(
        lax.dot_general(
            w_down, hidden, (((0,), (1,)), ((), ())), preferred_element_type=f32
        ).astype(jnp.bfloat16),
        "tp",
        scatter_dimension=0,
        tiled=True,
    ).astype(jnp.float32)
    return share.T


def body(
    tokens,
    memory,
    normalizer,
    stabilizer,
    first_gain,
    first_gate,
    first_up,
    first_down,
    mixer_gain,
    query_weight,
    key_weight,
    value_weight,
    input_weight,
    forget_weight,
    forget_bias,
    output_weight,
    last_gain,
    last_gate,
    last_up,
    last_down,
):
    f32 = jnp.float32
    model_width = first_gain.shape[0]
    rows, col_width = tokens.shape
    block = lax.all_gather(tokens, "tp", axis=1, tiled=True)
    first_share = gated_block(block, first_gain, first_gate, first_up, first_down, model_width)
    stream_one = (tokens.astype(f32) + 0.5 * first_share).astype(jnp.bfloat16)
    seq_count, head_count, value_size, key_size = memory.shape
    moved = lax.all_to_all(
        stream_one.reshape(rows, 1, col_width), "kv", split_axis=0, concat_axis=1, tiled=True
    )
    own_rows = lax.all_gather(moved, "tp", axis=2, tiled=True).reshape(seq_count, model_width)
    row_values = own_rows.astype(f32)
    scale = lax.rsqrt(jnp.mean(row_values * row_values, axis=1, keepdims=True) + EPS)
    cell_in = (row_values * mixer_gain).astype(jnp.bfloat16)
    query = (
        scale * jnp.dot(cell_in, query_weight, preferred_element_type=f32) * key_size ** (-0.5)
    ).reshape(seq_count, head_count, key_size)
    key = (scale * jnp.dot(cell_in, key_weight, preferred_element_type=f32)).reshape(
        seq_count, head_count, key_size
    )
    value = (scale * jnp.dot(cell_in, value_weight, preferred_element_type=f32)).reshape(
        seq_count, head_count, value_size
    )
    first_head = lax.axis_index("tp") * head_count
    input_all = scale * jnp.dot(cell_in, input_weight, preferred_element_type=f32)
    forget_all = scale * jnp.dot(cell_in, forget_weight, preferred_element_type=f32)
    input_pre = lax.dynamic_slice_in_dim(input_all, first_head, head_count, 1)
    log_forget = jax.nn.log_sigmoid(
        lax.dynamic_slice_in_dim(forget_all, first_head, head_count, 1) + forget_bias
    )
    carried = log_forget + stabilizer
    new_stabilizer = jnp.maximum(carried, input_pre)
    keep = jnp.exp(carried - new_stabilizer)
    admit = jnp.exp(input_pre - new_stabilizer)
    recalled = jnp.einsum("bhvd,bhd->bhv", memory, query, precision=lax.Precision.HIGHEST)
    match = jnp.sum(query * key, axis=-1)
    numer = keep[..., None] * recalled + (admit * match)[..., None] * value
    denom = keep * jnp.sum(normalizer * query, axis=-1) + admit * match
    cell_out = (
        (numer / jnp.maximum(jnp.abs(denom), 1.0)[..., None])
        .reshape(seq_count, head_count * value_size)
        .astype(jnp.bfloat16)
    )
    new_memory = (
        keep[..., None, None] * memory
        + admit[..., None, None] * value[..., :, None] * key[..., None, :]
    )
    new_normalizer = keep[..., None] * normalizer + admit[..., None] * key
    partial_heads = jnp.dot(cell_out, output_weight, preferred_element_type=f32)
    mixed = lax.psum(partial_heads.astype(jnp.bfloat16), "tp").astype(jnp.float32)
    rows_two = (row_values + mixed).astype(jnp.bfloat16)
    whole_two = lax.all_to_all(rows_two, "kv", split_axis=1, concat_axis=0, tiled=True)
    last_share = gated_block(whole_two, last_gain, last_gate, last_up, last_down, model_width)
    own_columns = lax.dynamic_slice_in_dim(
        whole_two, lax.axis_index("tp") * col_width, col_width, 1
    )
    result = (own_columns.astype(f32) + 0.5 * last_share).astype(jnp.bfloat16)
    return (result, new_memory, new_normalizer, new_stabilizer)


def tiles_fit(tokens, memory, first_down, kv_size, tp_size):
    rows, col_width = tokens.shape
    seqs, heads, value_size, key_size = memory.shape
    hidden = first_down.shape[0]
    return (
        col_width % 128 == 0
        and hidden % (128 * kv_size) == 0
        and seqs % 16 == 0
        and seqs * kv_size == rows
        and key_size % 128 == 0
        and value_size % 128 == 0
        and tp_size > 1
        and kv_size > 1
    )


def make_kernel(K, T, R, C, F, S, H, DK, DV, heads_all):
    f32, bf16 = jnp.float32, jnp.bfloat16
    W, FQ = C * T, F // K
    D = W * K
    remote_count = 4 * (T - 1) + 6 * (K - 1) + 2 * (K * T - 1)

    def kernel(
        tokens, normalizer, stabilizer, first_gain, mixer_gain, forget_bias, last_gain,
        memory, fg, fu, fd, wq, wk, wv, wi, wf, wo, lg, lu, ld,
        result, v_mem, norm_out, stab_out,
        send_sem, recv_sem, load_sem,
        v_fg, v_fu, v_fd, v_lg, v_lu, v_ld, v_qkv, v_wif, v_wo,
        *bufs,
    ):
        mlp_bufs = (bufs[0:9], bufs[9:18])
        s_one, rows_in, rows_val, cell_in, qkv, cell_out, part, part_in, two, two_in, s_two, keep_rows = bufs[18:]
        k = lax.axis_index("kv")
        t = lax.axis_index("tp")
        counter = [0]

        loads = {}

        def load(name, src, dst):
            i = len(loads)
            copy = pltpu.make_async_copy(src, dst, load_sem.at[i])
            copy.start()
            loads[name] = copy

        load("fg", fg, v_fg)
        load("fu", fu, v_fu)
        load("fd", fd, v_fd)
        load("wq", wq, v_qkv.at[:, pl.ds(0, H * DK)])
        load("wk", wk, v_qkv.at[:, pl.ds(H * DK, H * DK)])
        load("wv", wv, v_qkv.at[:, pl.ds(2 * H * DK, H * DV)])
        load("wi", wi, v_wif.at[pl.ds(0, heads_all), :])
        load("wf", wf, v_wif.at[pl.ds(heads_all, heads_all), :])
        load("mem", memory, v_mem)
        load("wo", wo, v_wo)
        load("lg", lg, v_lg)
        load("lu", lu, v_lu)
        load("ld", ld, v_ld)

        barrier = pltpu.get_barrier_semaphore()
        others = [(a, b) for a in range(K) for b in range(T) if a or b]
        for a, b in others:
            device = (lax.rem(k + a, K), lax.rem(t + b, T))
            pl.semaphore_signal(barrier, inc=1, device_id=device, device_id_type=MESH)
        pl.semaphore_wait(barrier, K * T - 1)

        def send(src, dst, device):
            i = counter[0]
            counter[0] += 1
            copy = pltpu.make_async_remote_copy(
                src_ref=src, dst_ref=dst, send_sem=send_sem.at[i], recv_sem=recv_sem.at[i],
                device_id=device, device_id_type=MESH,
            )
            copy.start()
            return copy

        started = []

        def tp_to(o):
            return (k, lax.rem(t + o, T))

        def kv_to(o):
            return (lax.rem(k + o, K), t)

        def tp_from(o):
            return lax.rem(t + (T - o), T)

        def kv_from(o):
            return lax.rem(k + (K - o), K)

        def cols(at, width):
            return pl.ds(pl.multiple_of(at * width, width), width)

        def exchange(piece, land):
            return {
                (a, b): send(
                    piece(lax.rem(k + a, K)), land.at[a * T + b], (lax.rem(k + a, K), lax.rem(t + b, T))
                )
                for a, b in others
            }

        def gain_at(gain, src):
            return gain[:, pl.ds(pl.multiple_of((k * T + src) * C, C), C)]

        def mlp(own, gain, vg, vu, vd, names, b, arrived=None):
            gath, scaled, sq_out, sq_in, gu_out, gu_in, hid_in, down_acc, down = b[:9]
            if arrived is None:
                copies = [send(own, gath.at[o], tp_to(o)) for o in range(1, T)]
                squares = jnp.zeros((R, C), f32)
                for o in range(0, T):
                    if o:
                        copies[o - 1].wait_recv()
                    src = tp_from(o)
                    values = (gath[o] if o else own[...]).astype(f32)
                    scaled[:, cols(src, C)] = (values * gain_at(gain, src)).astype(bf16)
                    squares = squares + values * values
                started.extend(copies)
                sq_out[...] = jnp.broadcast_to(jnp.sum(squares, axis=1, keepdims=True), (R, 128))
            else:
                first, land, copies = arrived
                for a in range(K):
                    row = pl.ds(pl.multiple_of(kv_from(a) * S, S), S)
                    squares = jnp.zeros((S, C), f32)
                    for o in range(T):
                        if a or o:
                            copies[a, o].wait_recv()
                        piece = land[a * T + o] if a or o else first
                        src = tp_from(o)
                        values = piece.astype(f32)
                        scaled[row, cols(src, C)] = (values * gain_at(gain, src)).astype(bf16)
                        squares = squares + values * values
                        if o == 0:
                            own[row, :] = piece
                    sq_out[row, :] = jnp.broadcast_to(jnp.sum(squares, axis=1, keepdims=True), (S, 128))
                started.extend(copies.values())
            total = sq_out[:, :1]
            sq_copies = [send(sq_out, sq_in.at[o], kv_to(o)) for o in range(1, K)]
            loads[names[0]].wait()
            loads[names[1]].wait()
            x = scaled[...]
            gu_copies = []
            for o in range(1, K):
                at = cols(lax.rem(k + o, K), FQ)
                gu_out[o, 0] = jnp.dot(x, vg[:, at], preferred_element_type=f32).astype(bf16)
                gu_out[o, 1] = jnp.dot(x, vu[:, at], preferred_element_type=f32).astype(bf16)
                gu_copies.append(send(gu_out.at[o], gu_in.at[o], kv_to(o)))
            at = cols(k, FQ)
            gate = jnp.dot(x, vg[:, at], preferred_element_type=f32)
            up = jnp.dot(x, vu[:, at], preferred_element_type=f32)
            for c in sq_copies:
                c.wait_recv()
            for o in range(1, K):
                total = total + sq_in[o][:, :1]
            scale = lax.rsqrt(total / D + EPS)
            for o in range(1, K):
                gu_copies[o - 1].wait_recv()
                gate = gate + gu_in[o, 0].astype(f32)
                up = up + gu_in[o, 1].astype(f32)
            gate = gate * scale
            up = up * scale
            mine = (gate / (1.0 + jnp.exp(-gate)) * up).astype(bf16)
            hid_in[0] = mine
            hid_copies = [send(hid_in.at[0], hid_in.at[o], kv_to(o)) for o in range(1, K)]
            loads[names[2]].wait()
            half = max(W // 2, 128)

            def rows_of(src):
                return pl.ds(pl.multiple_of(src * FQ, FQ), FQ)

            for o in range(K - 1):
                if o:
                    hid_copies[o - 1].wait_recv()
                row = rows_of(kv_from(o))
                for c in range(0, W, half):
                    term = jnp.dot(hid_in[o], vd[row, c:c + half], preferred_element_type=f32)
                    down_acc[:, c:c + half] = term + down_acc[:, c:c + half] if o else term
            hid_copies[K - 2].wait_recv()
            row = rows_of(kv_from(K - 1))
            out_copies = []
            for c in range(0, W, half):
                term = down_acc[:, c:c + half] + jnp.dot(hid_in[K - 1], vd[row, c:c + half], preferred_element_type=f32)
                for i in range(half // C):
                    down[c // C + i] = term[:, i * C:(i + 1) * C].astype(bf16)
            out_copies = [send(down.at[lax.rem(t + o, T)], gath.at[T + o], tp_to(o)) for o in range(1, T)]
            acc = down[t].astype(f32)
            for o in range(1, T):
                out_copies[o - 1].wait_recv()
                acc = acc + gath[T + o].astype(f32)
            started.extend(sq_copies + gu_copies + hid_copies + out_copies)
            return (own[...].astype(f32) + 0.5 * acc).astype(bf16)

        s_one[...] = mlp(tokens, first_gain, v_fg, v_fu, v_fd, ("fg", "fu", "fd"), mlp_bufs[0])

        def rows_for(group):
            return s_one.at[pl.ds(pl.multiple_of(group * S, S), S), :]

        gather = exchange(rows_for, rows_in)
        squares = jnp.zeros((S, C), f32)
        for a in range(K):
            for o in range(T):
                if a or o:
                    gather[a, o].wait_recv()
                piece = rows_in[a * T + o] if a or o else s_one[pl.ds(pl.multiple_of(k * S, S), S), :]
                values = piece.astype(f32)
                at = cols(kv_from(a) * T + tp_from(o), C)
                rows_val[:, at] = values
                cell_in[:, at] = (values * mixer_gain[:, at]).astype(bf16)
                squares = squares + values * values
        started.extend(gather.values())
        scale = lax.rsqrt(jnp.sum(squares, axis=1, keepdims=True) / D + EPS)
        for name in ("wq", "wk", "wv", "wi", "wf"):
            loads[name].wait()
        width = 2 * H * DK + H * DV

        def project(n, carry):
            at = cols(n, 128 * 2 if width % 256 == 0 else 128)
            qkv[:, at] = scale * jnp.dot(cell_in[...], v_qkv[:, at], preferred_element_type=f32)
            return carry

        lax.fori_loop(0, width // (256 if width % 256 == 0 else 128), project, 0)
        dims = (((1,), (1,)), ((), ()))
        gates = scale * lax.dot_general(cell_in[...], v_wif[...], dims, preferred_element_type=f32)
        lane = lax.broadcasted_iota(jnp.int32, gates.shape, 1)
        loads["mem"].wait()
        rowid = lax.broadcasted_iota(jnp.int32, (S, DV), 0)
        query = qkv[:, : H * DK] * DK ** (-0.5)
        key = qkv[:, H * DK : 2 * H * DK]
        value = qkv[:, 2 * H * DK :]
        hi = query.astype(bf16)
        lo = (query - hi.astype(f32)).astype(bf16)
        both = jnp.concatenate([hi, lo], axis=0)
        step = 4 if S % 4 == 0 else 1

        def recall(i, acc):
            acc = list(acc)
            for h in range(H):
                for j in range(step):
                    m = v_mem[i * step + j, h].astype(bf16)
                    r = lax.dot_general(both[:, h * DK : (h + 1) * DK], m, dims, preferred_element_type=f32)
                    acc[h] = jnp.where(rowid == i * step + j, r[:S] + r[S:], acc[h])
            return tuple(acc)

        recalled = lax.fori_loop(0, S // step, recall, tuple(jnp.zeros((S, DV), f32) for _ in range(H)))
        eye = lax.broadcasted_iota(jnp.int32, (S, S), 0) == lax.broadcasted_iota(jnp.int32, (S, S), 1)
        outer = []
        for h in range(H):
            at = t * H + h
            input_pre = jnp.sum(jnp.where(lane == at, gates, 0.0), axis=1, keepdims=True)
            pre = jnp.sum(jnp.where(lane == at + heads_all, gates, 0.0), axis=1, keepdims=True)
            pre = pre + forget_bias[:, h : h + 1]
            held_stab = jnp.sum(jnp.where(eye, stabilizer[h : h + 1, :], 0.0), axis=1, keepdims=True)
            log_forget = jnp.minimum(pre, 0.0) - jnp.log1p(jnp.exp(-jnp.abs(pre)))
            carried = log_forget + held_stab
            new_stab = jnp.maximum(carried, input_pre)
            keep = jnp.exp(carried - new_stab)
            admit = jnp.exp(input_pre - new_stab)
            stab_out[h : h + 1, :] = jnp.sum(jnp.where(eye, new_stab, 0.0), axis=0, keepdims=True)
            keep_rows[h] = jnp.broadcast_to(keep, (S, DK))
            qh = query[:, h * DK : (h + 1) * DK]
            kh = key[:, h * DK : (h + 1) * DK]
            vh = value[:, h * DV : (h + 1) * DV]
            old_norm = normalizer[:, h, :]
            match = jnp.sum(qh * kh, axis=1, keepdims=True)
            held = jnp.sum(qh * old_norm, axis=1, keepdims=True)
            norm_out[:, h, :] = keep * old_norm + admit * kh
            admitted = admit * vh
            a_hi = admitted.astype(bf16).astype(f32)
            k_hi = kh.astype(bf16).astype(f32)
            left = jnp.concatenate([a_hi, admitted - a_hi, a_hi], axis=0).T.astype(bf16)
            right = jnp.concatenate([k_hi, k_hi, kh - k_hi], axis=0)
            outer.append((left, right))
            numer = keep * recalled[h] + (admit * match) * vh
            denom = keep * held + admit * match
            cell_out[:, h * DV : (h + 1) * DV] = (numer / jnp.maximum(jnp.abs(denom), 1.0)).astype(bf16)

        loads["wo"].wait()

        def spread(j, carry):
            for c in range(0, T):
                at = pl.ds(pl.multiple_of(j * W + c * C, C), C)
                part[c, j] = jnp.dot(cell_out[...], v_wo[:, at], preferred_element_type=f32).astype(bf16)
            return carry

        lax.fori_loop(0, K, spread, 0)
        mix = [send(part.at[lax.rem(t + o, T)], part_in.at[o], tp_to(o)) for o in range(1, T)]
        row3 = lax.rem(lax.broadcasted_iota(jnp.int32, (3 * S, DK), 0), S)

        def update(i, carry):
            for h in range(H):
                left, right = outer[h]
                for j in range(step):
                    n = i * step + j
                    term = jnp.dot(left, jnp.where(row3 == n, right, 0.0).astype(bf16), preferred_element_type=f32)
                    v_mem[n, h] = keep_rows[h, pl.ds(n, 1), :] * v_mem[n, h] + term
            return carry

        lax.fori_loop(0, S // step, update, 0)
        mixed = part[t].astype(f32)
        for o in range(1, T):
            mix[o - 1].wait_recv()
            mixed = mixed + part_in[o].astype(f32)
        for j in range(K):
            at = cols(j * T + t, C)
            two[j] = (rows_val[:, at] + mixed[j]).astype(bf16)
        back = exchange(lambda group: two.at[group], two_in)
        started.extend(mix)
        result[...] = mlp(
            s_two, last_gain, v_lg, v_lu, v_ld, ("lg", "lu", "ld"), mlp_bufs[1], (two[k], two_in, back)
        )
        for c in started:
            c.wait_send()

    mlp_scratch = [
        pltpu.VMEM((2 * T, R, C), bf16),
        pltpu.VMEM((R, W), bf16),
        pltpu.VMEM((R, 128), f32),
        pltpu.VMEM((K, R, 128), f32),
        pltpu.VMEM((K, 2, R, FQ), bf16),
        pltpu.VMEM((K, 2, R, FQ), bf16),
        pltpu.VMEM((K, R, FQ), bf16),
        pltpu.VMEM((R, W), f32),
        pltpu.VMEM((T, R, C), bf16),
    ]

    def scratch():
        return [
            pltpu.SemaphoreType.DMA((remote_count,)),
            pltpu.SemaphoreType.DMA((remote_count,)),
            pltpu.SemaphoreType.DMA((13,)),
            pltpu.VMEM((W, F), bf16),
            pltpu.VMEM((W, F), bf16),
            pltpu.VMEM((F, W), bf16),
            pltpu.VMEM((W, F), bf16),
            pltpu.VMEM((W, F), bf16),
            pltpu.VMEM((F, W), bf16),
            pltpu.VMEM((D, 2 * H * DK + H * DV), bf16),
            pltpu.VMEM((2 * heads_all, D), bf16),
            pltpu.VMEM((H * DV, D), bf16),
            *mlp_scratch,
            *mlp_scratch,
            pltpu.VMEM((R, C), bf16),
            pltpu.VMEM((K * T, S, C), bf16),
            pltpu.VMEM((S, D), f32),
            pltpu.VMEM((S, D), bf16),
            pltpu.VMEM((S, 2 * H * DK + H * DV), f32),
            pltpu.VMEM((S, H * DV), bf16),
            pltpu.VMEM((T, K, S, C), bf16),
            pltpu.VMEM((T, K, S, C), bf16),
            pltpu.VMEM((K, S, C), bf16),
            pltpu.VMEM((K * T, S, C), bf16),
            pltpu.VMEM((R, C), bf16),
            pltpu.VMEM((H, S, DK), f32),
        ]

    return kernel, scratch


def fused_body(
    tokens, memory, normalizer, stabilizer, first_gain, first_gate, first_up, first_down,
    mixer_gain, query_weight, key_weight, value_weight, input_weight, forget_weight,
    forget_bias, output_weight, last_gain, last_gate, last_up, last_down,
):
    f32 = jnp.float32
    kv_size, tp_size = lax.axis_size("kv"), lax.axis_size("tp")
    R, C = tokens.shape
    S, H, DV, DK = memory.shape
    F = first_down.shape[0]
    kernel, scratch = make_kernel(
        kv_size, tp_size, R, C, F, S, H, DK, DV, input_weight.shape[1]
    )
    vmem, anyspace = pl.BlockSpec(memory_space=pltpu.VMEM), pl.BlockSpec(memory_space=pl.ANY)
    shape = jax.ShapeDtypeStruct
    result, new_memory, new_normalizer, new_stabilizer = pl.pallas_call(
        kernel,
        out_shape=(
            shape((R, C), jnp.bfloat16),
            pltpu.VMEM((S, H, DV, DK), f32),
            shape((S, H, DK), f32),
            shape((H, S), f32),
        ),
        in_specs=[vmem] * 7 + [anyspace] * 13,
        out_specs=(vmem,) * 4,
        scratch_shapes=scratch(),
        compiler_params=pltpu.CompilerParams(
            collective_id=0, has_side_effects=True, vmem_limit_bytes=57 * 2**20
        ),
    )(
        tokens, normalizer, stabilizer.T, first_gain[None], mixer_gain[None], forget_bias[None], last_gain[None],
        memory, first_gate, first_up, first_down, query_weight, key_weight, value_weight,
        input_weight.T, forget_weight.T, output_weight, last_gate, last_up, last_down,
    )
    return result, new_memory, new_normalizer, new_stabilizer.T


def solution(mesh):
    in_specs = (
        P(None, ("kv", "tp")),
        P("kv", "tp", None, None),
        P("kv", "tp", None),
        P("kv", "tp"),
        P(),
        P("kv", "tp"),
        P("kv", "tp"),
        P("tp", "kv"),
        P(),
        P(None, "tp"),
        P(None, "tp"),
        P(None, "tp"),
        P(),
        P(),
        P("tp"),
        P("tp", None),
        P(),
        P("kv", "tp"),
        P("kv", "tp"),
        P("tp", "kv"),
    )
    out_specs = (
        P(None, ("kv", "tp")),
        P("kv", "tp", None, None),
        P("kv", "tp", None),
        P("kv", "tp"),
    )
    kv_size, tp_size = mesh.shape["kv"], mesh.shape["tp"]

    def chosen(tokens, memory, *rest):
        fits = tiles_fit(tokens, memory, rest[5], kv_size, tp_size)
        return (fused_body if fits else body)(tokens, memory, *rest)

    return jax.shard_map(chosen, mesh=mesh, in_specs=in_specs, out_specs=out_specs, check_vma=False)
```
